32 devices in a mesh: rep: 2 (over x), fs: 8 (over z, y), tp: 2 (over core).
Axes of the slice: x: 2, y: 2, z: 4, core: 2. Of those that a mesh axis runs over, the one named last changes fastest.
Arguments:
- layer_in: bfloat16 [16384, 2048], P(('rep', 'fs'), 'tp'), may hold values from -60 to 60
- mix_gain: bfloat16 [2048], P('tp'), may hold values from 0.099609375 to 1.8984375
- pool_weight: float32 [4, 512, 512], P('tp', None, 'fs'), may hold values from -0.25 to 0.25
- pool_scale: float32 [4, 512], P('tp'), may hold values from 0.1 to 1.9
- out_weight: float32 [2048, 2048], P('tp', 'fs'), may hold values from -0.125 to 0.125
- out_scale: float32 [2048], P('tp'), may hold values from 0.1 to 1.9
- channel_gain: bfloat16 [2048], P('tp'), may hold values from 0.099609375 to 1.8984375
- up_weight: float32 [2048, 2816], P('fs', 'tp'), may hold values from -0.125 to 0.125
- up_scale: float32 [2816], P('tp'), may hold values from 0.1 to 1.9
- gate_weight: float32 [2048, 2816], P('fs', 'tp'), may hold values from -0.125 to 0.125
- gate_scale: float32 [2816], P('tp'), may hold values from 0.1 to 1.9
- conv_weight: float32 [3, 2816], P(None, 'tp'), may hold values from -3 to 3
- down_weight: float32 [2816, 2048], P('tp', 'fs'), may hold values from -0.109375 to 0.109375
- down_scale: float32 [2048], P('tp'), may hold values from 0.1 to 1.9
Outputs:
- layer_out: bfloat16 [16384, 2048], P(('rep', 'fs'), 'tp')
The draws below stay inside these ranges and needn't reach their ends.
All inputs are finite; a program needn't handle non-finite values.
Results may differ from the reference program's by a relative error of at most 0.0095.
Values may be sent and summed in bfloat16 or wider, within the bound.
A program may use at most 128 MiB of HBM per device.

```python
import jax
import jax.numpy as jnp
from jax import lax

D = 2048
FF = 2816
GROUPS = 4
GROUP_DIM = 512
LENGTH = 256
TOKENS = 16384
N_FS = 8
N_TP = 2


def draw_layer_in(key, part):
    first, second, third = jax.random.split(jax.random.fold_in(key, 11), 3)
    rising = jnp.exp(jnp.log(3.0) * jnp.arange(D, dtype=jnp.float32) / D)
    column = rising * jax.random.uniform(second, (D,), jnp.float32, 0.5, 1.5)
    base = jnp.clip(jax.random.normal(first, (TOKENS, D), jnp.float32), -4.0, 4.0)
    row_scale = jnp.exp(jax.random.uniform(third, (TOKENS, 1), jnp.float32, jnp.log(0.3), jnp.log(3.0)))
    return (base * column[None] * row_scale).astype(jnp.bfloat16)


def block_scale(stream_key, extent, shards, low, top_value):
    def one(dim, parts):
        heights = jax.random.uniform(jax.random.fold_in(jax.random.fold_in(stream_key, 6), dim), (parts,), jnp.float32, low / len(shards), top_value / len(shards))
        return jnp.repeat(jnp.exp(heights), extent[dim] // parts).reshape((-1,) + (1,) * (len(extent) - dim - 1))

    level = one(*shards[0])
    for cut in shards[1:]:
        level = level * one(*cut)
    return level


def bell_draw(own_key, shape, spread, reach, cuts=(), kind=jnp.bfloat16):
    factor_of = block_scale(own_key, shape, cuts, -0.22, 0.18) if cuts else 1.0
    values = jax.random.normal(own_key, shape, jnp.float32) * spread * factor_of
    return jnp.minimum(jnp.maximum(values, -reach), reach).astype(kind)


def setup_inputs(seed: int = 0) -> dict:
    arg_keys = jax.random.split(jax.random.key(seed), 15)
    layer_in = draw_layer_in(jax.random.fold_in(arg_keys[14], 71), 0)
    mix_gain = jnp.clip(1.0 + 0.18 * jax.random.normal(arg_keys[1], (D,), jnp.float32), 0.099609375, 1.8984375).astype(jnp.bfloat16)
    pool_weight = bell_draw(arg_keys[2], (GROUPS, GROUP_DIM, GROUP_DIM), GROUP_DIM ** -0.5, 0.25, ((0, 2), (2, 8)), jnp.float32)
    pool_scale = jnp.clip(1.0 + 0.18 * jax.random.normal(arg_keys[3], (GROUPS, GROUP_DIM), jnp.float32), 0.1, 1.9)
    out_weight = bell_draw(arg_keys[4], (D, D), D ** -0.5, 0.125, ((0, 2), (1, 8)), jnp.float32)
    out_scale = jnp.clip(1.0 + 0.18 * jax.random.normal(arg_keys[5], (D,), jnp.float32), 0.1, 1.9)
    channel_gain = jnp.clip(1.0 + 0.18 * jax.random.normal(arg_keys[6], (D,), jnp.float32), 0.099609375, 1.8984375).astype(jnp.bfloat16)
    up_weight = bell_draw(arg_keys[7], (D, FF), D ** -0.5, 0.125, ((0, 8), (1, 2)), jnp.float32)
    up_scale = jnp.clip(1.0 + 0.18 * jax.random.normal(arg_keys[8], (FF,), jnp.float32), 0.1, 1.9)
    gate_weight = bell_draw(arg_keys[9], (D, FF), D ** -0.5, 0.125, ((0, 8), (1, 2)), jnp.float32)
    gate_scale = jnp.clip(1.0 + 0.18 * jax.random.normal(arg_keys[10], (FF,), jnp.float32), 0.1, 1.9)
    conv_weight = bell_draw(arg_keys[11], (3, FF), 0.577, 3.0, ((1, 2),), jnp.float32)
    down_weight = bell_draw(arg_keys[12], (FF, D), FF ** -0.5, 0.109375, ((0, 2), (1, 8)), jnp.float32)
    down_scale = jnp.clip(1.0 + 0.18 * jax.random.normal(arg_keys[13], (D,), jnp.float32), 0.1, 1.9)
    return dict(layer_in=layer_in, mix_gain=mix_gain, pool_weight=pool_weight, pool_scale=pool_scale, out_weight=out_weight, out_scale=out_scale, channel_gain=channel_gain, up_weight=up_weight, up_scale=up_scale, gate_weight=gate_weight, gate_scale=gate_scale, conv_weight=conv_weight, down_weight=down_weight, down_scale=down_scale)


EPS = 1e-06

def settle(values):
    return lax.optimization_barrier(values.astype(jnp.bfloat16)).astype(jnp.float32)

def band_table(length, window):
    rows = lax.broadcasted_iota(jnp.int32, (length, length), 0)
    cols = lax.broadcasted_iota(jnp.int32, (length, length), 1)
    lower = jnp.maximum(rows - window // 2, 0)
    upper = jnp.minimum(rows - window // 2 + window, length)
    inside = (cols >= lower) & (cols < upper)
    count = (upper[:, :1] - lower[:, :1]).astype(jnp.float32)
    return (inside.astype(jnp.bfloat16), count)

def partial_sums(left, right):
    part = left.shape[1] // N_TP
    total = jnp.zeros((left.shape[0], right.shape[1]), jnp.float32)
    for index in range(N_TP):
        piece = jnp.dot(left[:, index * part:(index + 1) * part], right[index * part:(index + 1) * part], preferred_element_type=jnp.float32)
        total = total + settle(piece)
    return total

def block_layer(block_in, mix_gain, pool_bf, pool_scale, out_bf, out_scale, channel_gain, up_bf, up_scale, gate_bf, gate_scale, conv_weight, down_bf, down_scale):
    rows = block_in.shape[0]
    seqs = rows // LENGTH
    x32 = block_in.astype(jnp.float32)
    normed = settle(x32 * lax.rsqrt(lax.optimization_barrier(jnp.mean(x32 * x32, axis=1, keepdims=True)) + EPS) * mix_gain.astype(jnp.float32))
    grouped_in = normed.reshape(seqs, LENGTH, GROUPS, GROUP_DIM)
    outputs = []
    for group in range(GROUPS):
        band, count = band_table(LENGTH, 2 ** (group + 1))
        piece = grouped_in[:, :, group, :]
        total = jnp.einsum('ij,sjc->sic', band.astype(jnp.float32), piece)
        outputs.append(settle(total / count[None] - piece))
    pooled = jnp.stack(outputs, axis=2)
    grouped = jnp.einsum('slgc,gcd->slgd', pooled, pool_bf.astype(jnp.float32)) * pool_scale[None, None]
    grouped = settle(grouped).astype(jnp.bfloat16).reshape(rows, D)
    mixer_sum = partial_sums(grouped, out_bf)
    middle = (x32 + mixer_sum * out_scale[None]).astype(jnp.bfloat16)
    m32 = middle.astype(jnp.float32)
    chan_normed = (m32 * lax.rsqrt(lax.optimization_barrier(jnp.mean(m32 * m32, axis=1, keepdims=True)) + EPS) * channel_gain.astype(jnp.float32)).astype(jnp.bfloat16)
    lifted = settle(jnp.dot(chan_normed, up_bf, preferred_element_type=jnp.float32) * up_scale[None])
    gated = jnp.dot(chan_normed, gate_bf, preferred_element_type=jnp.float32) * gate_scale[None]
    padded = jnp.pad(lifted.reshape(seqs, LENGTH, FF), ((0, 0), (1, 1), (0, 0)))
    conv = conv_weight[0] * padded[:, :-2] + conv_weight[1] * padded[:, 1:-1] + conv_weight[2] * padded[:, 2:]
    hidden = (jax.nn.gelu(conv).reshape(rows, FF) * gated).astype(jnp.bfloat16)
    chan_sum = partial_sums(hidden, down_bf)
    return (m32 + chan_sum * down_scale[None]).astype(jnp.bfloat16)

def reference(layer_in, mix_gain, pool_weight, pool_scale, out_weight, out_scale, channel_gain, up_weight, up_scale, gate_weight, gate_scale, conv_weight, down_weight, down_scale):
    pool_bf = pool_weight.astype(jnp.bfloat16)
    out_bf = out_weight.astype(jnp.bfloat16)
    up_bf = up_weight.astype(jnp.bfloat16)
    gate_bf = gate_weight.astype(jnp.bfloat16)
    down_bf = down_weight.astype(jnp.bfloat16)
    blocks = layer_in.reshape(N_FS, TOKENS // N_FS, D)

    def one_block(block_in):
        return block_layer(block_in, mix_gain, pool_bf, pool_scale, out_bf, out_scale, channel_gain, up_bf, up_scale, gate_bf, gate_scale, conv_weight, down_bf, down_scale)
    return lax.map(one_block, blocks).reshape(TOKENS, D)
```

```python
import functools

import jax
import jax.numpy as jnp
from jax import lax
from jax.experimental import pallas as pl
from jax.experimental.pallas import tpu as pltpu
from jax.sharding import PartitionSpec as P

LENGTH = 256


EPS = 1e-06


def band_table(length, window):
    rows = lax.broadcasted_iota(jnp.int32, (length, length), 0)
    cols = lax.broadcasted_iota(jnp.int32, (length, length), 1)
    lower = jnp.maximum(rows - window // 2, 0)
    upper = jnp.minimum(rows - window // 2 + window, length)
    inside = (cols >= lower) & (cols < upper)
    count = (upper[:, :1] - lower[:, :1]).astype(jnp.float32)
    return (inside.astype(jnp.bfloat16), count)


def pool_group(piece, window):
    band, count = band_table(piece.shape[1], window)
    total = jnp.einsum("ij,sjc->sic", band, piece, preferred_element_type=jnp.float32)
    return (total / count[None] - piece.astype(jnp.float32)).astype(jnp.bfloat16)


def times_rows(left, rows):
    return lax.dot_general(
        left, rows, (((1,), (1,)), ((), ())), preferred_element_type=jnp.float32
    )


def assemble_kernel(outer, inner, height, swap, *refs):
    far, near = refs[:outer], refs[outer : 2 * outer]
    rest = refs[2 * outer : -2]
    out_ref, sems = refs[-2:]
    spot = lax.axis_index("fs")
    column, lane = spot // inner, spot % inner
    side = lax.axis_index("rep")
    copies = []

    def put(source, row, count, slot, offset):
        start = pl.multiple_of(slot * height + offset, 16)
        copies.append(
            pltpu.make_async_copy(
                source.at[pl.ds(row, count)], out_ref.at[pl.ds(start, count)], sems.at[len(copies)]
            )
        )
        copies[-1].start()

    for step in range(outer):
        home = lax.rem(column + outer - step, outer) * inner
        for source, group, slot in ((far, 0, home + lane), (near, 1, home + inner - 1 - lane)):
            if swap:
                put(source[step], 0, swap, slot, side * swap)
                put(rest[group], step * swap, swap, slot, (1 - side) * swap)
            put(source[step], swap, height - 2 * swap, slot, 2 * swap)
    for copy in copies:
        copy.wait()


def gather_all(shards, outer, inner, reps):
    side = lax.axis_index("rep")
    pair = [(a * inner + b, a * inner + inner - 1 - b) for a in range(outer) for b in range(inner)]
    across = [(0, 1), (1, 0)]

    def ring(step):
        return [
            (a * inner + b, (a + step) % outer * inner + b)
            for a in range(outer)
            for b in range(inner)
        ]

    swaps, spares, owns = [], [], []
    for shard in shards:
        swap = (shard.shape[0] * 3 // 8) // 16 * 16 if reps == 2 else 0
        first, second, common = shard[:swap], shard[swap : 2 * swap], shard[2 * swap :]
        swaps.append(swap)
        spares.append(jnp.where(side == 0, second, first))
        owns.append(jnp.concatenate([jnp.where(side == 0, first, second), common]))
    count = len(shards)
    far, near, rest = [None] * count, [None] * count, [()] * count
    before = ()
    for stage in range(count + 2):
        along, pairs, cross = stage, stage - 1, stage - 2
        sent = [None, None, None]
        if along < count:
            sent[0] = owns[along]
        if 0 <= pairs < count:
            sent[1] = far[pairs][1:]
        if 0 <= cross < count and swaps[cross]:
            swap = swaps[cross]
            sent[2] = (
                jnp.concatenate([p[:swap] for p in far[cross][1:]]),
                jnp.concatenate([p[:swap] for p in near[cross]]),
            )
        sent, _ = lax.optimization_barrier((sent, before))
        before = []
        if sent[0] is not None:
            moved = [lax.ppermute(sent[0], "fs", ring(step)) for step in range(1, outer)]
            near[along] = [lax.ppermute(sent[0], "fs", pair)]
            far[along] = [owns[along]] + moved
            before += moved + near[along]
        if sent[1] is not None:
            moved = [lax.ppermute(piece, "fs", pair) for piece in sent[1]]
            near[pairs] = near[pairs] + moved
            before += moved
        if sent[2] is not None:
            moved = [lax.ppermute(piece, "rep", across) for piece in sent[2]]
            rest[cross] = (moved[0], moved[1])
            before += moved

    def assemble(index, result):
        height, width = shards[index].shape
        (far_in, near_in, rest_in), result = lax.optimization_barrier(
            ((far[index], near[index], rest[index]), result)
        )
        if rest_in:
            rest_in = (jnp.concatenate([spares[index], rest_in[0]]), rest_in[1])
        full = pl.pallas_call(
            functools.partial(assemble_kernel, outer, inner, height, swaps[index]),
            out_shape=jax.ShapeDtypeStruct((outer * inner * height, width), shards[index].dtype),
            in_specs=[pl.BlockSpec(memory_space=pl.ANY)] * (2 * outer + len(rest_in)),
            out_specs=pl.BlockSpec(memory_space=pltpu.VMEM),
            scratch_shapes=[pltpu.SemaphoreType.DMA((6 * outer,))],
            cost_estimate=pl.CostEstimate(flops=2_000_000_000, bytes_accessed=0, transcendentals=0),
        )(*far_in, *near_in, *rest_in)
        return full, result

    return assemble


def per_device(
    outer,
    inner,
    reps,
    layer_in,
    mix_gain,
    pool_weight,
    pool_scale,
    out_weight,
    out_scale,
    channel_gain,
    up_weight,
    up_scale,
    gate_weight,
    gate_scale,
    conv_weight,
    down_weight,
    down_scale,
):
    rows, half = layer_in.shape
    seqs = rows // LENGTH
    width = half * lax.axis_size("tp")
    hidden_width = up_weight.shape[1]
    local_groups = pool_weight.shape[0]
    group_width = half // local_groups
    core = lax.axis_index("tp")
    other_core = [(0, 1), (1, 0)]

    pool_rows = jnp.transpose(pool_weight.astype(jnp.bfloat16), (2, 0, 1)).reshape(-1, half)
    out_rows = jnp.swapaxes(out_weight.astype(jnp.bfloat16), 0, 1)
    mix_height = pool_rows.shape[0]
    assemble = gather_all(
        (
            jnp.concatenate([pool_rows, out_rows]),
            up_weight.astype(jnp.bfloat16),
            gate_weight.astype(jnp.bfloat16),
            jnp.swapaxes(down_weight.astype(jnp.bfloat16), 0, 1),
        ),
        outer,
        inner,
        reps,
    )

    def tp_exchange(terms):
        sent = terms.astype(jnp.bfloat16)
        low, high = sent[:, :half], sent[:, half:]
        arrived = lax.ppermute(jnp.where(core == 0, high, low), "tp", other_core)
        kept = jnp.where(core == 0, low, high)
        return kept.astype(jnp.float32) + arrived.astype(jnp.float32)

    x32 = layer_in.astype(jnp.float32)
    squares = lax.psum(jnp.sum(x32 * x32, axis=1), "tp")
    normed = (
        x32 * lax.rsqrt(squares / width + EPS)[:, None] * mix_gain.astype(jnp.float32)[None]
    ).astype(jnp.bfloat16)
    mix_full, normed = assemble(0, normed)
    mix_full = mix_full.reshape(outer * inner, -1, half)
    pool_full = mix_full[:, :mix_height].reshape(group_width, half)
    out_full = mix_full[:, mix_height:].reshape(width, half)
    grouped = []
    for local in range(local_groups):
        window = jnp.left_shift(jnp.int32(1), core * local_groups + local + 1)
        part = slice(local * group_width, (local + 1) * group_width)
        pooled = pool_group(normed[:, part].reshape(seqs, LENGTH, group_width), window)
        linear = times_rows(pooled.reshape(rows, group_width), pool_full[:, part])
        grouped.append((linear * pool_scale[local][None]).astype(jnp.bfloat16))
    mixer_sum = tp_exchange(times_rows(jnp.concatenate(grouped, axis=1), out_full))
    middle = (x32 + mixer_sum * out_scale[None]).astype(jnp.bfloat16)
    m32 = middle.astype(jnp.float32)
    middle_squares = lax.psum(jnp.sum(m32 * m32, axis=1), "tp")
    own_normed = (
        m32
        * lax.rsqrt(middle_squares / width + EPS)[:, None]
        * channel_gain.astype(jnp.float32)[None]
    ).astype(jnp.bfloat16)
    far_normed = lax.ppermute(own_normed, "tp", other_core)
    chan_normed = jnp.concatenate(
        [jnp.where(core == 0, own_normed, far_normed), jnp.where(core == 0, far_normed, own_normed)],
        axis=1,
    )
    up_full, chan_normed = assemble(1, chan_normed)
    lifted_raw = jnp.dot(chan_normed, up_full, preferred_element_type=jnp.float32)
    lifted = (lifted_raw * up_scale[None]).astype(jnp.bfloat16)
    gate_full, lifted = assemble(2, lifted)
    gated_raw = jnp.dot(chan_normed, gate_full, preferred_element_type=jnp.float32)
    padded = jnp.pad(
        lifted.reshape(seqs, LENGTH, hidden_width).astype(jnp.float32), ((0, 0), (1, 1), (0, 0))
    )
    conv = (
        conv_weight[0] * padded[:, :-2]
        + conv_weight[1] * padded[:, 1:-1]
        + conv_weight[2] * padded[:, 2:]
    )
    hidden = (
        jax.nn.gelu(conv).reshape(rows, hidden_width) * (gated_raw * gate_scale[None])
    ).astype(jnp.bfloat16)
    down_full, hidden = assemble(3, hidden)
    chan_sum = tp_exchange(times_rows(hidden, down_full))
    return (m32 + chan_sum * down_scale[None]).astype(jnp.bfloat16)


def solution(mesh):
    placed = (
        P(("rep", "fs"), "tp"),
        P("tp"),
        P("tp", None, "fs"),
        P("tp", None),
        P("tp", "fs"),
        P("tp"),
        P("tp"),
        P("fs", "tp"),
        P("tp"),
        P("fs", "tp"),
        P("tp"),
        P(None, "tp"),
        P("tp", "fs"),
        P("tp"),
    )
    shards = mesh.shape["fs"]
    inner = 2
    body = functools.partial(per_device, shards // inner, inner, mesh.shape["rep"])
    return jax.shard_map(
        body, mesh=mesh, in_specs=placed, out_specs=P(("rep", "fs"), "tp"), check_vma=False
    )
```
